32 devices in a mesh: sp: 16 (over z, y, x), tp: 2 (over core).
Axes of the slice: x: 2, y: 2, z: 4, core: 2. Of those that a mesh axis runs over, the one named last changes fastest.
Arguments:
- features: bfloat16 [8192, 4096], P('sp', 'tp'), may hold values from -6 to 6
- weight_value: bfloat16 [4096, 1024], P(None, 'tp'), may hold values from -0.09375 to 0.09375
- weight_gate: bfloat16 [4096, 1024], P(None, 'tp'), may hold values from -0.09375 to 0.09375
- weight_out: bfloat16 [4096, 1024], P(None, 'tp'), may hold values from -0.1875 to 0.1875
- conv_taps: float32 [31, 1024], P(None, 'tp'), may hold values from -6 to 6
- norm_gain: float32 [1024], P('tp'), may hold values from 0.1 to 1.9
- out_grad: bfloat16 [8192, 4096], P('sp', 'tp'), may hold values from -6 to 6
Outputs:
- value_grad: float32 [8192, 1024], P('sp', 'tp')
- gate_grad: float32 [8192, 1024], P('sp', 'tp')
- value_wgrad: float32 [4096, 1024], P('sp', 'tp')
- gate_wgrad: float32 [4096, 1024], P('sp', 'tp')
- out_wgrad: float32 [4096, 1024], P('sp', 'tp')
- taps_grad: float32 [31, 1024], P(None, 'tp')
- gain_grad: float32 [1024], P('tp')
The draws below stay inside these ranges and needn't reach their ends.
All inputs are finite; a program needn't handle non-finite values.
Results may differ from the reference program's by a relative error of at most 0.0057.
Values may be sent and summed in bfloat16 or wider, within the bound.
A program may use at most 192 MiB of HBM per device.

```python
import math
import jax
import jax.numpy as jnp
from jax import lax

D = 4096
CH = 1024
KW = 31
TOKENS = 8192


def draw_conv_taps(key, part):
    base_key = jax.random.fold_in(key, 11)
    first_key, second_key, third_key = jax.random.split(base_key, 3)
    base = jnp.clip(jax.random.normal(first_key, (KW, CH), jnp.float32), -3.5, 3.5)
    spread = jnp.exp(jax.random.uniform(second_key, (CH,), jnp.float32, -0.7, 0.7))
    upper_big = jax.random.bernoulli(third_key)
    lower_half = jnp.arange(CH) < CH // 2
    block_scale = jnp.where(lower_half == upper_big, 3.5, 1.0)
    return base * spread * block_scale / math.sqrt(KW)


def strengthened(entries, own_key, source, target, shards_of, factor):
    owner, partner = [(jnp.arange(entries.shape[position]) // (entries.shape[position] // shards_of)).reshape([-1 if axis == position else 1 for axis in range(entries.ndim)]) for position in (source, target)]
    chosen = jax.random.permutation(own_key, shards_of)[partner]
    strong = (owner == chosen) | (owner == (partner + shards_of // 2) % shards_of)
    return jnp.where(strong, factor * entries, entries)


def shard_levels(key, shape, cuts, low, high):
    loudness = 1.0
    for position, blocks in cuts:
        heights = jax.random.uniform(jax.random.fold_in(jax.random.fold_in(key, 6), position), (blocks,), jnp.float32, low / len(cuts), high / len(cuts))
        loudness = loudness * jnp.repeat(jnp.exp(heights), shape[position] // blocks).reshape((-1,) + (1,) * (len(shape) - 1 - position))
    return loudness


def bell_draw(own_key, shape, deviation, most, cuts=(), held_as=jnp.bfloat16):
    result = deviation * jax.random.normal(own_key, shape, jnp.float32)
    if cuts:
        result = result * shard_levels(own_key, shape, cuts, -0.22, 0.18)
    return jnp.clip(result, -most, most).astype(held_as)


def noise_with(key, shape, scale, bound, shards, heavy, dtype=jnp.bfloat16):
    array = scale * jax.random.normal(key, shape, jnp.float32)
    if shards:
        array = array * shard_levels(key, shape, shards, -0.22, 0.18)
    return jnp.clip(strengthened(array, jax.random.fold_in(key, 3), *heavy), -bound, bound).astype(dtype)


def setup_inputs(seed: int = 0) -> dict:
    keys = jax.random.split(jax.random.key(seed), 8)
    return {
        "features": noise_with(keys[0], (TOKENS, D), 1.0, 6.0, ((0, 16), (1, 2)), (0, 1, 16, 2.0)),
        "weight_value": bell_draw(keys[1], (D, CH), D ** -0.5, 0.09375, ((1, 2),)),
        "weight_gate": bell_draw(keys[2], (D, CH), D ** -0.5, 0.09375, ((1, 2),)),
        "weight_out": bell_draw(keys[3], (D, CH), CH ** -0.5, 0.1875, ((1, 2),)),
        "conv_taps": draw_conv_taps(jax.random.fold_in(keys[7], 71), 0),
        "norm_gain": jnp.clip(1.0 + 0.18 * jax.random.normal(keys[5], (CH,), jnp.float32), 0.1, 1.9),
        "out_grad": noise_with(keys[6], (TOKENS, D), 1.0, 6.0, ((0, 16), (1, 2)), (0, 1, 16, 2.0)),
    }


NORM_EPS = 1e-05

def over_tokens(left_rows, right_rows):
    return lax.dot_general(left_rows, right_rows, (((0,), (0,)), ((), ())), preferred_element_type=jnp.float32)

def reference(features, weight_value, weight_gate, weight_out, conv_taps, norm_gain, out_grad):
    half_width = KW // 2
    seq_total = features.shape[0]
    value_half = jnp.dot(features, weight_value, preferred_element_type=jnp.float32).astype(jnp.bfloat16)
    gate_half = jnp.dot(features, weight_gate, preferred_element_type=jnp.float32).astype(jnp.bfloat16)
    value_half, gate_half = lax.optimization_barrier((value_half, gate_half))
    value_pre = value_half.astype(jnp.float32)
    gate_pre = gate_half.astype(jnp.float32)
    gate_sig = jax.nn.sigmoid(gate_pre)
    mixed_half = lax.optimization_barrier((value_pre * gate_sig).astype(jnp.bfloat16))
    padded = jnp.pad(mixed_half.astype(jnp.float32), ((half_width, half_width), (0, 0)))
    conv_out = jnp.zeros((seq_total, CH), jnp.float32)
    for offset in range(KW):
        conv_out = conv_out + conv_taps[offset] * padded[offset:offset + seq_total]
    mean_row = lax.optimization_barrier(jnp.sum(conv_out, axis=-1, keepdims=True)) / CH
    var_row = lax.optimization_barrier(jnp.sum(conv_out * conv_out, axis=-1, keepdims=True)) / CH - mean_row * mean_row
    inv_std = lax.rsqrt(var_row + NORM_EPS)
    normed = (conv_out - mean_row) * inv_std
    pre_act = normed * norm_gain
    act_sig = jax.nn.sigmoid(pre_act)
    act_half = (pre_act * act_sig).astype(jnp.bfloat16)
    act_grad = jnp.dot(out_grad, weight_out, preferred_element_type=jnp.float32)
    out_wgrad = over_tokens(out_grad, act_half)
    pre_grad = act_grad * act_sig * (1.0 + pre_act * (1.0 - act_sig))
    gain_grad = lax.optimization_barrier(jnp.sum(pre_grad * normed, axis=0))
    norm_grad = pre_grad * norm_gain
    first_mom = lax.optimization_barrier(jnp.sum(norm_grad, axis=-1, keepdims=True)) / CH
    second_mom = lax.optimization_barrier(jnp.sum(norm_grad * normed, axis=-1, keepdims=True)) / CH
    conv_grad = inv_std * (norm_grad - first_mom - normed * second_mom)
    grad_ext = jnp.pad(conv_grad, ((half_width, half_width), (0, 0)))
    mixed_grad = jnp.zeros((seq_total, CH), jnp.float32)
    taps_rows = []
    for offset in range(KW):
        begin = 2 * half_width - offset
        mixed_grad = mixed_grad + conv_taps[offset] * grad_ext[begin:begin + seq_total]
        taps_rows.append(lax.optimization_barrier(jnp.sum(conv_grad * padded[offset:offset + seq_total], axis=0)))
    taps_grad = jnp.stack(taps_rows)
    value_grad = mixed_grad * gate_sig
    gate_grad = mixed_grad * value_pre * gate_sig * (1.0 - gate_sig)
    value_wgrad = over_tokens(features, value_grad.astype(jnp.bfloat16))
    gate_wgrad = over_tokens(features, gate_grad.astype(jnp.bfloat16))
    return (value_grad, gate_grad, value_wgrad, gate_wgrad, out_wgrad, taps_grad, gain_grad)
```

```python
import jax
import jax.numpy as jnp
from jax import lax
from jax.sharding import PartitionSpec as P

NORM_EPS = 1e-05


def with_halo(block, sides, width):
    for axis, dim in sides:
        count = lax.axis_size(axis)
        forward = [(i, i + 1) for i in range(count - 1)]
        backward = [(target, source) for source, target in forward]
        low = lax.ppermute(
            lax.slice_in_dim(block, block.shape[dim] - width, None, axis=dim), axis, forward
        )
        high = lax.ppermute(lax.slice_in_dim(block, 0, width, axis=dim), axis, backward)
        block = jnp.concatenate([low, block, high], axis=dim)
    return block


def make_term(left_rows, right_rows):
    return lax.dot_general(
        left_rows, right_rows, (((0,), (0,)), ((), ())), preferred_element_type=jnp.float32
    )


def bit_of(axis, bit):
    return (lax.axis_index(axis) >> bit) & 1


def exchange(block, axis, bit):
    count = lax.axis_size(axis)
    return lax.ppermute(block, axis, [(i, i ^ (1 << bit)) for i in range(count)])


def both_halves(block, axis):
    other = exchange(block, axis, 0)
    first = lax.axis_index(axis) == 0
    return jnp.where(
        first,
        jnp.concatenate([block, other], axis=1),
        jnp.concatenate([other, block], axis=1),
    )


def butterfly_scatter(term, order):
    rows, columns = term.shape
    left = sorted(order)
    own_rows = rows >> len(left)
    total = term
    for bit in order:
        place = left.index(bit)
        low = own_rows << place
        high = rows // (2 * low)
        view = total.reshape(high, 2, low, columns)
        mine = bit_of("sp", bit)
        away = lax.dynamic_index_in_dim(view, 1 - mine, 1, keepdims=False)
        kept = lax.dynamic_index_in_dim(view, mine, 1, keepdims=False)
        got = exchange(away.astype(jnp.bfloat16), "sp", bit)
        total = kept.astype(jnp.float32) + got.astype(jnp.float32)
        rows //= 2
        left.remove(bit)
    return total.reshape(rows, columns)


def scatter_sum(left_rows, right_rows):
    term = make_term(left_rows, right_rows).astype(jnp.bfloat16)
    bits = list(range((lax.axis_size("sp") - 1).bit_length()))
    turn, rest = bits[:3], bits[3:]
    lanes = 128
    groups = term.shape[1] // lanes
    chunks = []
    begin = 0
    for k in range(len(turn)):
        width = lanes * ((groups - begin // lanes) // (len(turn) - k))
        piece = term[:, begin : begin + width]
        chunks.append(butterfly_scatter(piece, turn[k:] + turn[:k] + rest))
        begin += width
    return jnp.concatenate(chunks, axis=1)


def butterfly_sum(block):
    for bit in range((lax.axis_size("sp") - 1).bit_length()):
        block = block + exchange(block, "sp", bit)
    return block


def on_device(features, weight_value, weight_gate, weight_out, conv_taps, norm_gain, out_grad):
    whole_inputs, whole_cotangent = (
        both_halves(features, "tp"),
        both_halves(out_grad, "tp"),
    )
    value_half = jnp.dot(whole_inputs, weight_value, preferred_element_type=jnp.float32).astype(
        jnp.bfloat16
    )
    gate_half = jnp.dot(whole_inputs, weight_gate, preferred_element_type=jnp.float32).astype(
        jnp.bfloat16
    )
    value_half, gate_half = lax.optimization_barrier((value_half, gate_half))
    value_pre = value_half.astype(jnp.float32)
    gate_pre = gate_half.astype(jnp.float32)
    gate_sig = jax.nn.sigmoid(gate_pre)
    mixed_half = lax.optimization_barrier((value_pre * gate_sig).astype(jnp.bfloat16))
    tap_count = conv_taps.shape[0]
    half_width = tap_count // 2
    row_count = mixed_half.shape[0]
    channels = mixed_half.shape[1] * lax.axis_size("tp")
    extended = with_halo(mixed_half, (("sp", 0),), half_width).astype(jnp.float32)
    conv_out = jnp.zeros(mixed_half.shape, jnp.float32)
    for offset in range(tap_count):
        conv_out = conv_out + conv_taps[offset] * extended[offset : offset + row_count]
    row_sum, row_square = lax.psum(
        (jnp.sum(conv_out, axis=-1), jnp.sum(conv_out * conv_out, axis=-1)), "tp"
    )
    mean_row = row_sum[:, None] / channels
    var_row = row_square[:, None] / channels - mean_row * mean_row
    inv_std = lax.rsqrt(var_row + NORM_EPS)
    normed = (conv_out - mean_row) * inv_std
    pre_act = normed * norm_gain
    act_sig = jax.nn.sigmoid(pre_act)
    act_half = (pre_act * act_sig).astype(jnp.bfloat16)
    act_grad = jnp.dot(whole_cotangent, weight_out, preferred_element_type=jnp.float32)
    pre_grad = act_grad * act_sig * (1.0 + pre_act * (1.0 - act_sig))
    gain_part = jnp.sum(pre_grad * normed, axis=0)
    norm_grad = pre_grad * norm_gain
    first_sum, second_sum = lax.psum(
        (jnp.sum(norm_grad, axis=-1), jnp.sum(norm_grad * normed, axis=-1)), "tp"
    )
    first_mom = first_sum[:, None] / channels
    second_mom = second_sum[:, None] / channels
    conv_grad = inv_std * (norm_grad - first_mom - normed * second_mom)
    grad_ext = with_halo(conv_grad, (("sp", 0),), half_width)
    mixed_grad = jnp.zeros(conv_grad.shape, jnp.float32)
    taps_rows = []
    for offset in range(tap_count):
        begin = 2 * half_width - offset
        mixed_grad = mixed_grad + conv_taps[offset] * grad_ext[begin : begin + row_count]
        taps_rows.append(jnp.sum(conv_grad * extended[offset : offset + row_count], axis=0))
    small = butterfly_sum(jnp.stack(taps_rows + [gain_part]))
    taps_grad, gain_grad = small[:tap_count], small[tap_count]
    value_grad = mixed_grad * gate_sig
    gate_grad = mixed_grad * value_pre * gate_sig * (1.0 - gate_sig)
    value_low = value_grad.astype(jnp.bfloat16)
    gate_low = gate_grad.astype(jnp.bfloat16)
    out_wgrad = scatter_sum(whole_cotangent, act_half)
    both_low = jnp.concatenate([value_low, gate_low], axis=1)
    joined = scatter_sum(whole_inputs, both_low)
    split_at = value_low.shape[1]
    value_wgrad = joined[:, :split_at]
    gate_wgrad = joined[:, split_at:]
    return (value_grad, gate_grad, value_wgrad, gate_wgrad, out_wgrad, taps_grad, gain_grad)


def solution(mesh):
    in_specs = (
        P("sp", "tp"),
        P(None, "tp"),
        P(None, "tp"),
        P(None, "tp"),
        P(None, "tp"),
        P("tp"),
        P("sp", "tp"),
    )
    out_specs = (
        P("sp", "tp"),
        P("sp", "tp"),
        P("sp", "tp"),
        P("sp", "tp"),
        P("sp", "tp"),
        P(None, "tp"),
        P("tp"),
    )
    return jax.shard_map(
        on_device, mesh=mesh, in_specs=in_specs, out_specs=out_specs, check_vma=False
    )
```

```python
import functools

import jax
import jax.numpy as jnp
from jax import lax
from jax.experimental import pallas as pl
from jax.experimental.pallas import tpu as pltpu
from jax.sharding import PartitionSpec as P

NORM_EPS = 1e-05


def with_halo(block, sides, width):
    for axis, dim in sides:
        count = lax.axis_size(axis)
        forward = [(i, i + 1) for i in range(count - 1)]
        backward = [(target, source) for source, target in forward]
        low = lax.ppermute(
            lax.slice_in_dim(block, block.shape[dim] - width, None, axis=dim), axis, forward
        )
        high = lax.ppermute(lax.slice_in_dim(block, 0, width, axis=dim), axis, backward)
        block = jnp.concatenate([low, block, high], axis=dim)
    return block


def make_term(left_rows, right_rows):
    return lax.dot_general(
        left_rows, right_rows, (((0,), (0,)), ((), ())), preferred_element_type=jnp.float32
    )


def bit_of(axis, bit):
    return (lax.axis_index(axis) >> bit) & 1


def exchange(block, axis, bit):
    count = lax.axis_size(axis)
    return lax.ppermute(block, axis, [(i, i ^ (1 << bit)) for i in range(count)])


def both_halves(block, axis):
    other = exchange(block, axis, 0)
    first = lax.axis_index(axis) == 0
    return jnp.where(
        first,
        jnp.concatenate([block, other], axis=1),
        jnp.concatenate([other, block], axis=1),
    )


def scatter_kernel(bits, widths, *refs):
    terms = refs[: len(widths)]
    small = refs[len(widths)]
    outs = refs[len(widths) + 1 : 2 * len(widths) + 1]
    small_out = refs[2 * len(widths) + 1]
    scratch = refs[2 * len(widths) + 2 :]
    got, sent = scratch[:bits], scratch[bits : 2 * bits - 1]
    small_got, small_cur, send_sem, recv_sem, small_send, small_recv = scratch[2 * bits - 1 :]
    me, core = lax.axis_index("sp"), lax.axis_index("tp")
    mine = [(me // (1 << bit)) % 2 for bit in range(bits)]
    partner = [me + (1 << bit) * (1 - 2 * mine[bit]) for bit in range(bits)]

    barrier = pltpu.get_barrier_semaphore()
    for bit in range(bits):
        pl.semaphore_signal(
            barrier, inc=1, device_id=(partner[bit], core), device_id_type=pl.DeviceIdType.MESH
        )
    pl.semaphore_wait(barrier, bits)

    turn = min(3, bits)
    groups = []
    for which, width in enumerate(widths):
        for begin in range(0, width, 128):
            k = len(groups) % turn
            order = list(range(turn))[k:] + list(range(turn))[:k] + list(range(turn, bits))
            groups.append((which, pl.ds(begin, 128), order))

    def remote(src, dst, send, recv, bit):
        return pltpu.make_async_remote_copy(
            src_ref=src,
            dst_ref=dst,
            send_sem=send,
            recv_sem=recv,
            device_id=(partner[bit], core),
            device_id_type=pl.DeviceIdType.MESH,
        )

    down = list(range(bits - 1, -1, -1))

    def summed(group, stage, value):
        which, columns, order = groups[group]
        total = terms[which][tuple(value[bit] for bit in down) + (slice(None), columns)]
        total = total.astype(jnp.float32)
        for s in range(stage):
            left = sorted(order[s + 1 :], reverse=True)
            total += got[s][(group,) + tuple(value[bit] for bit in left)].astype(jnp.float32)
        return total

    copies = {}

    def start(group, stage):
        which, columns, order = groups[group]
        bit = order[stage]
        if stage == 0:
            place = tuple(1 - mine[b] if b == bit else slice(None) for b in down)
            src = terms[which].at[place + (slice(None), columns)]
        else:
            copies[group, stage - 1].wait_recv()
            left = sorted(order[stage + 1 :], reverse=True)
            value = {b: mine[b] for b in order[:stage]}
            value[bit] = 1 - mine[bit]
            src = sent[stage - 1].at[group]
            for number in range(1 << len(left)):
                for position, b in enumerate(left):
                    value[b] = (number >> (len(left) - 1 - position)) & 1
                place = tuple(value[b] for b in left)
                src[place] = summed(group, stage, value).astype(jnp.bfloat16)
        copy = remote(
            src, got[stage].at[group], send_sem.at[group, stage], recv_sem.at[group, stage], bit
        )
        copy.start()
        copies[group, stage] = copy

    def finish(group):
        which, columns, order = groups[group]
        copies[group, bits - 1].wait_recv()
        value = {b: mine[b] for b in order}
        outs[which][:, columns] = summed(group, bits, value)

    small_copies = []

    def small_step(stage):
        if stage:
            small_copies[stage - 1].wait_recv()
            before = small if stage == 1 else small_cur.at[stage - 2]
            now = small_out if stage == bits else small_cur.at[stage - 1]
            now[...] = before[...] + small_got[stage - 1]
        if stage < bits:
            copy = remote(
                small if stage == 0 else small_cur.at[stage - 1],
                small_got.at[stage],
                small_send.at[stage],
                small_recv.at[stage],
                stage,
            )
            copy.start()
            small_copies.append(copy)

    tasks = []
    for group in range(len(groups)):
        wave = group // turn
        tasks.append((wave - 1.0, 0, group))
        tasks += [(wave + float(stage), -stage, group) for stage in range(1, bits + 1)]
    tasks += [(0.5 + 1.0 * stage, 9, stage) for stage in range(1, bits + 1)]
    small_step(0)
    for _, kind, number in sorted(tasks):
        if kind == 9:
            small_step(number)
        elif -kind < bits:
            start(number, -kind)
        else:
            finish(number)
    for copy in list(copies.values()) + small_copies:
        copy.wait_send()


def scatter_all(terms, small):
    count = lax.axis_size("sp")
    bits = (count - 1).bit_length()
    own_rows = terms[0].shape[0] // count
    widths = [term.shape[1] for term in terms]
    groups = sum(widths) // 128
    views = [term.reshape((2,) * bits + (own_rows, term.shape[1])) for term in terms]
    vmem = pl.BlockSpec(memory_space=pltpu.VMEM)

    def block(left):
        return pltpu.VMEM((groups,) + (2,) * left + (own_rows, 128), jnp.bfloat16)

    results = pl.pallas_call(
        functools.partial(scatter_kernel, bits, widths),
        out_shape=[jax.ShapeDtypeStruct((own_rows, width), jnp.float32) for width in widths]
        + [jax.ShapeDtypeStruct(small.shape, jnp.float32)],
        in_specs=[vmem] * (len(views) + 1),
        out_specs=[vmem] * (len(views) + 1),
        scratch_shapes=[block(bits - 1 - stage) for stage in range(bits)]
        + [block(bits - 1 - stage) for stage in range(1, bits)]
        + [
            pltpu.VMEM((bits,) + small.shape, jnp.float32),
            pltpu.VMEM((bits,) + small.shape, jnp.float32),
            pltpu.SemaphoreType.DMA((groups, bits)),
            pltpu.SemaphoreType.DMA((groups, bits)),
            pltpu.SemaphoreType.DMA((bits,)),
            pltpu.SemaphoreType.DMA((bits,)),
        ],
        compiler_params=pltpu.CompilerParams(
            collective_id=3, has_side_effects=True, vmem_limit_bytes=58 * 1024 * 1024
        ),
        name="scatter_all",
    )(*views, small)
    return results[:-1], results[-1]


def on_device(features, weight_value, weight_gate, weight_out, conv_taps, norm_gain, out_grad):
    whole_inputs, whole_cotangent = (
        both_halves(features, "tp"),
        both_halves(out_grad, "tp"),
    )
    value_half = jnp.dot(whole_inputs, weight_value, preferred_element_type=jnp.float32).astype(
        jnp.bfloat16
    )
    gate_half = jnp.dot(whole_inputs, weight_gate, preferred_element_type=jnp.float32).astype(
        jnp.bfloat16
    )
    value_half, gate_half = lax.optimization_barrier((value_half, gate_half))
    value_pre = value_half.astype(jnp.float32)
    gate_pre = gate_half.astype(jnp.float32)
    gate_sig = jax.nn.sigmoid(gate_pre)
    mixed_half = lax.optimization_barrier((value_pre * gate_sig).astype(jnp.bfloat16))
    tap_count = conv_taps.shape[0]
    half_width = tap_count // 2
    row_count = mixed_half.shape[0]
    channels = mixed_half.shape[1] * lax.axis_size("tp")
    extended = with_halo(mixed_half, (("sp", 0),), half_width).astype(jnp.float32)
    conv_out = jnp.zeros(mixed_half.shape, jnp.float32)
    for offset in range(tap_count):
        conv_out = conv_out + conv_taps[offset] * extended[offset : offset + row_count]
    row_sum, row_square = lax.psum(
        (jnp.sum(conv_out, axis=-1), jnp.sum(conv_out * conv_out, axis=-1)), "tp"
    )
    mean_row = row_sum[:, None] / channels
    var_row = row_square[:, None] / channels - mean_row * mean_row
    inv_std = lax.rsqrt(var_row + NORM_EPS)
    normed = (conv_out - mean_row) * inv_std
    pre_act = normed * norm_gain
    act_sig = jax.nn.sigmoid(pre_act)
    act_half = (pre_act * act_sig).astype(jnp.bfloat16)
    act_grad = jnp.dot(whole_cotangent, weight_out, preferred_element_type=jnp.float32)
    pre_grad = act_grad * act_sig * (1.0 + pre_act * (1.0 - act_sig))
    gain_part = jnp.sum(pre_grad * normed, axis=0)
    norm_grad = pre_grad * norm_gain
    first_sum, second_sum = lax.psum(
        (jnp.sum(norm_grad, axis=-1), jnp.sum(norm_grad * normed, axis=-1)), "tp"
    )
    first_mom = first_sum[:, None] / channels
    second_mom = second_sum[:, None] / channels
    conv_grad = inv_std * (norm_grad - first_mom - normed * second_mom)
    grad_ext = with_halo(conv_grad, (("sp", 0),), half_width)
    mixed_grad = jnp.zeros(conv_grad.shape, jnp.float32)
    taps_rows = []
    for offset in range(tap_count):
        begin = 2 * half_width - offset
        mixed_grad = mixed_grad + conv_taps[offset] * grad_ext[begin : begin + row_count]
        taps_rows.append(jnp.sum(conv_grad * extended[offset : offset + row_count], axis=0))
    small = jnp.stack(taps_rows + [gain_part])
    value_grad = mixed_grad * gate_sig
    gate_grad = mixed_grad * value_pre * gate_sig * (1.0 - gate_sig)
    value_low = value_grad.astype(jnp.bfloat16)
    gate_low = gate_grad.astype(jnp.bfloat16)
    out_term = make_term(whole_cotangent, act_half).astype(jnp.bfloat16)
    both_low = jnp.concatenate([value_low, gate_low], axis=1)
    both_term = make_term(whole_inputs, both_low).astype(jnp.bfloat16)
    (out_wgrad, joined), small = scatter_all([out_term, both_term], small)
    taps_grad, gain_grad = small[:tap_count], small[tap_count]
    split_at = value_low.shape[1]
    value_wgrad = joined[:, :split_at]
    gate_wgrad = joined[:, split_at:]
    return (value_grad, gate_grad, value_wgrad, gate_wgrad, out_wgrad, taps_grad, gain_grad)


def solution(mesh):
    in_specs = (
        P("sp", "tp"),
        P(None, "tp"),
        P(None, "tp"),
        P(None, "tp"),
        P(None, "tp"),
        P("tp"),
        P("sp", "tp"),
    )
    out_specs = (
        P("sp", "tp"),
        P("sp", "tp"),
        P("sp", "tp"),
        P("sp", "tp"),
        P("sp", "tp"),
        P(None, "tp"),
        P("tp"),
    )
    return jax.shard_map(
        on_device, mesh=mesh, in_specs=in_specs, out_specs=out_specs, check_vma=False
    )
```
